32 devices in a mesh: grp: 2 (over x), fs: 4 (over z), tp: 4 (over y, core).
Axes of the slice: x: 2, y: 2, z: 4, core: 2. Of those that a mesh axis runs over, the one named last changes fastest.
Arguments:
- stream: bfloat16 [2048, 2048], P(('grp', 'fs'), 'tp'), parts along dimension 0, may hold values from -80 to 80
- mixed: bfloat16 [2048, 2048], P(('grp', 'fs'), 'tp'), parts along dimension 0, may hold values from -6 to 6
- out_weight: bfloat16 [2048, 2048], P('fs', 'tp'), may hold values from -0.125 to 0.125
- norm_gain: bfloat16 [2048], P('tp'), may hold values from 0.099609375 to 1.8984375
- up_weight: bfloat16 [2048, 8192], P('fs', 'tp'), may hold values from -0.125 to 0.125
- down_weight: bfloat16 [8192, 2048], P('tp', 'fs'), may hold values from -0.09375 to 0.09375
Outputs:
- result: bfloat16 [2048, 2048], P(('grp', 'fs'), 'tp'), parts along dimension 0
The draws below stay inside these ranges and needn't reach their ends.
There are 2 independent parts, one for each index of `grp`. The reference program is written for one: setup_inputs(seed, part) draws one part's arguments, and reference() takes and returns one part's arrays. A program takes and returns all parts, laid end to end along the dimension named above; an argument that names none is the same for every part. Nothing has to cross between parts.
All inputs are finite; a program needn't handle non-finite values.
Results may differ from the reference program's by a relative error of at most 0.01.
Values may be sent and summed in bfloat16 or wider, within the bound.
No kernel may reach another device: no remote copies, remote signals or barrier semaphores. Data moves between devices by JAX's collectives and lax.ppermute only.
A program may use at most 64 MiB of HBM per device.

```python
import jax
import jax.numpy as jnp
from jax import lax

D = 2048
FF = 8192
TOKENS = 1024


def draw_stream(key, part):
    base_key = jax.random.fold_in(key, 11)
    first, second, third = jax.random.split(base_key, 3)
    position = jnp.arange(D, dtype=jnp.float32) / max(D - 1, 1)
    column_scale = jnp.exp(position * jnp.log(4.0)) * jax.random.uniform(second, (D,), jnp.float32, 0.6, 1.4)
    row_scale = jnp.exp(jax.random.uniform(third, (TOKENS, 1), jnp.float32, jnp.log(0.5), jnp.log(2.0)))
    values = jnp.clip(jax.random.normal(first, (TOKENS, D), jnp.float32), -6.0, 6.0) * row_scale
    return (values * column_scale).astype(jnp.bfloat16)


def strengthened(drawn, key, source, target, parts, factor):
    owner, partner = [(jnp.arange(drawn.shape[dim]) // (drawn.shape[dim] // parts)).reshape([-1 if axis == dim else 1 for axis in range(drawn.ndim)]) for dim in (source, target)]
    chosen = jax.random.permutation(key, parts)[partner]
    strong = (owner == chosen) | (owner == (partner + parts // 2) % parts)
    return jnp.where(strong, factor * drawn, drawn)


def levels(key, extent, cuts, low, largest):
    factor_of = 1.0
    for dim, blocks in cuts:
        heights = jax.random.uniform(jax.random.fold_in(jax.random.fold_in(key, 6), dim), (blocks,), jnp.float32, low / len(cuts), largest / len(cuts))
        factor_of = factor_of * jnp.repeat(jnp.exp(heights), extent[dim] // blocks).reshape((-1,) + (1,) * (len(extent) - 1 - dim))
    return factor_of


def scatter_about(own_key, shape, deviation, limit, pieces=(), kind=jnp.bfloat16):
    entries = jax.random.normal(own_key, shape, jnp.float32) * deviation
    if len(pieces) > 0:
        entries = levels(own_key, shape, pieces, -0.22, 0.18) * entries
    return jnp.clip(entries, min=-limit, max=limit).astype(kind)


def noise_with(rng, extent, scale, bound, pieces, heavy, held_as=jnp.bfloat16):
    array = scale * jax.random.normal(rng, extent, jnp.float32)
    if pieces:
        array = array * levels(rng, extent, pieces, -0.22, 0.18)
    return jnp.clip(strengthened(array, jax.random.fold_in(rng, 3), *heavy), -bound, bound).astype(held_as)


def setup_inputs(seed: int = 0, part: int = 0) -> dict:
    keys = jax.random.split(jax.random.key(seed), 7)
    part_keys = jax.random.split(jax.random.fold_in(keys[6], part), 7)
    stream = draw_stream(jax.random.fold_in(jax.random.fold_in(keys[6], part), 71), part)
    mixed = scatter_about(part_keys[1], (TOKENS, D), 1.0, 6.0, ((0, 4), (1, 4)))
    out_weight = scatter_about(keys[2], (D, D), D ** -0.5, 0.125, ((0, 4), (1, 4)))
    norm_gain = jnp.clip(1.0 + 0.18 * jax.random.normal(keys[3], (D,), jnp.float32), 0.099609375, 1.8984375).astype(jnp.bfloat16)
    up_weight = scatter_about(keys[4], (D, FF), D ** -0.5, 0.125, ((0, 4), (1, 4)))
    down_weight = noise_with(keys[5], (FF, D), FF ** -0.5, 0.09375, ((0, 4), (1, 4)), (0, 1, 4, 2.0))
    return dict(stream=stream, mixed=mixed, out_weight=out_weight, norm_gain=norm_gain, up_weight=up_weight, down_weight=down_weight)


epsilon = 1e-06

def reference(stream, mixed, out_weight, norm_gain, up_weight, down_weight):
    projected = jnp.dot(mixed, out_weight, preferred_element_type=jnp.float32)
    resid = (stream.astype(jnp.float32) + projected).astype(jnp.bfloat16)
    widened = resid.astype(jnp.float32)
    energy = lax.optimization_barrier(jnp.mean(widened * widened, axis=-1, keepdims=True))
    normed = (widened * lax.rsqrt(energy + epsilon) * norm_gain.astype(jnp.float32)).astype(jnp.bfloat16)
    up_values = jnp.dot(normed, up_weight, preferred_element_type=jnp.float32)
    activated = jnp.square(jax.nn.relu(up_values)).astype(jnp.bfloat16)
    branch = jnp.dot(activated, down_weight, preferred_element_type=jnp.float32)
    return (widened + branch).astype(jnp.bfloat16)
```

```python
import jax
import jax.numpy as jnp
from jax import lax
from jax.sharding import PartitionSpec as P

epsilon = 1e-06


def fold_product(left, portion):
    return jnp.dot(left, portion, preferred_element_type=jnp.float32)


def gathered_weights(stream, mixed, out_weight, norm_gain, up_weight, down_weight):
    mixed_whole = lax.all_gather(mixed, "tp", axis=1, tiled=True)
    projected = fold_product(mixed_whole, lax.all_gather(out_weight, "fs", axis=0, tiled=True))
    resid = (stream.astype(jnp.float32) + projected).astype(jnp.bfloat16)
    widened = resid.astype(jnp.float32)
    resid_whole, gain_whole = (
        lax.all_gather(resid, "tp", axis=1, tiled=True),
        lax.all_gather(norm_gain, "tp", axis=0, tiled=True),
    )
    stream_wide = resid_whole.astype(jnp.float32)
    energy = jnp.mean(stream_wide * stream_wide, axis=1, keepdims=True)
    normed_whole = (
        stream_wide * lax.rsqrt(energy + epsilon) * gain_whole.astype(jnp.float32)
    ).astype(jnp.bfloat16)
    up_full = lax.all_gather(up_weight, "fs", axis=0, tiled=True)
    up_values = fold_product(normed_whole, up_full)
    activated = jnp.square(jax.nn.relu(up_values)).astype(jnp.bfloat16)
    partials = fold_product(activated, lax.all_gather(down_weight, "fs", axis=1, tiled=True))
    branch = lax.psum_scatter(partials, "tp", scatter_dimension=1, tiled=True)
    return (widened + branch).astype(jnp.bfloat16)


def gathered_tokens(parts, stream, mixed, out_weight, norm_gain, up_weight, down_weight):
    tokens, width = stream.shape
    depth, half = width, width // 2
    part, row, column = lax.axis_index("grp"), lax.axis_index("fs"), lax.axis_index("tp")
    shifts = range(1, parts)

    def along_rows(value, shift):
        return lax.ppermute(value, "fs", [(i, (i + shift) % parts) for i in range(parts)])

    def across_parts(value):
        return lax.ppermute(value, "grp", [(0, 1), (1, 0)])

    def across_columns(value, flip):
        return lax.ppermute(value, "tp", [(i, i ^ flip) for i in range(parts)])

    def pick(stacked, index):
        return lax.dynamic_index_in_dim(stacked, index, 0, keepdims=False)

    def exchange(value, axis):
        return lax.all_to_all(value, axis, 0, 0)

    out_mine = lax.dynamic_slice_in_dim(out_weight, part * half, half, 1)
    out_near = [along_rows(out_mine, shift) for shift in shifts]
    mixed_all = exchange(jnp.broadcast_to(mixed, (parts, *mixed.shape)), "tp")
    out_far = [across_parts(piece) for piece in out_near]
    own_block = pick(mixed_all, row)
    near = fold_product(own_block, out_mine)
    far = fold_product(own_block, lax.dynamic_slice_in_dim(out_weight, (1 - part) * half, half, 1))
    for shift, a, b in zip(shifts, out_near, out_far):
        block = pick(mixed_all, (row - shift) % parts)
        near += fold_product(block, a)
        far += fold_product(block, b)
    first = part == 0
    projected = jnp.concatenate([jnp.where(first, near, far), jnp.where(first, far, near)], 1)
    resid = (stream.astype(jnp.float32) + projected).astype(jnp.bfloat16)
    widened = resid.astype(jnp.float32)
    scaled = (widened * norm_gain.astype(jnp.float32)).astype(jnp.bfloat16)
    power = jnp.sum(widened * widened, axis=1)
    power_all = exchange(jnp.broadcast_to(power.reshape(-1, 128), (parts, tokens // 128, 128)), "tp")
    energy = jnp.sum(power_all, axis=0).reshape(tokens, 1) / (parts * width)

    up_near = exchange(
        jnp.swapaxes(
            lax.dynamic_index_in_dim(up_weight.reshape(depth, parts, 2, -1), part, 2, keepdims=False), 0, 1
        ),
        "fs",
    )
    up_far = across_parts(up_near)
    down_near = exchange(
        lax.dynamic_index_in_dim(down_weight.reshape(parts, 2, -1, width), part, 1, keepdims=False), "fs"
    )
    down_far = across_parts(down_near)

    by_row = jnp.concatenate([scaled] + [along_rows(scaled, shift) for shift in shifts], 0)
    by_pair = across_columns(by_row, 2)
    features = [by_row, None, by_pair, None]
    features[1] = across_columns(by_row, 1)
    features[3] = across_columns(by_pair, 1)

    hidden = []
    for stacked in (up_near, up_far):
        value = sum(fold_product(features[j], pick(stacked, column ^ j)) for j in range(parts))
        hidden.append(jnp.square(jax.nn.relu(value)).astype(jnp.bfloat16))
    sums = [
        fold_product(hidden[0], pick(down_near, column ^ j)) + fold_product(hidden[1], pick(down_far, column ^ j))
        for j in range(parts)
    ]
    got = [across_columns(sums[j].astype(jnp.bfloat16), 1) for j in (1, 3)]
    keep = sums[0] + got[0].astype(jnp.float32)
    give = sums[2] + got[1].astype(jnp.float32)
    keep += across_columns(give.astype(jnp.bfloat16), 2).astype(jnp.float32)
    keep = keep.reshape(parts, tokens, width)
    branch = keep[0]
    for shift in shifts:
        branch += along_rows(keep[shift].astype(jnp.bfloat16), -shift).astype(jnp.float32)
    return (widened + branch / (energy + epsilon)).astype(jnp.bfloat16)


def solution(mesh):
    shape = mesh.shape
    placed = (
        P(("grp", "fs"), "tp"),
        P(("grp", "fs"), "tp"),
        P("fs", "tp"),
        P("tp"),
        P("fs", "tp"),
        P("tp", "fs"),
    )

    def body(*blocks):
        if shape["grp"] == 2 and shape["fs"] == 4 and shape["tp"] == 4:
            return gathered_tokens(shape["fs"], *blocks)
        return gathered_weights(*blocks)

    return jax.shard_map(
        body, mesh=mesh, in_specs=placed, out_specs=P(("grp", "fs"), "tp"), check_vma=False
    )
```

```python
import functools

import jax
import jax.numpy as jnp
from jax import lax
from jax.experimental import pallas as pl
from jax.experimental.pallas import tpu as pltpu
from jax.sharding import PartitionSpec as P

epsilon = 1e-06


def fold_product(left, portion):
    return jnp.dot(left, portion, preferred_element_type=jnp.float32)


def gathered_weights(stream, mixed, out_weight, norm_gain, up_weight, down_weight):
    mixed_whole = lax.all_gather(mixed, "tp", axis=1, tiled=True)
    projected = fold_product(mixed_whole, lax.all_gather(out_weight, "fs", axis=0, tiled=True))
    resid = (stream.astype(jnp.float32) + projected).astype(jnp.bfloat16)
    widened = resid.astype(jnp.float32)
    resid_whole, gain_whole = (
        lax.all_gather(resid, "tp", axis=1, tiled=True),
        lax.all_gather(norm_gain, "tp", axis=0, tiled=True),
    )
    stream_wide = resid_whole.astype(jnp.float32)
    energy = jnp.mean(stream_wide * stream_wide, axis=1, keepdims=True)
    normed_whole = (
        stream_wide * lax.rsqrt(energy + epsilon) * gain_whole.astype(jnp.float32)
    ).astype(jnp.bfloat16)
    up_full = lax.all_gather(up_weight, "fs", axis=0, tiled=True)
    up_values = fold_product(normed_whole, up_full)
    activated = jnp.square(jax.nn.relu(up_values)).astype(jnp.bfloat16)
    partials = fold_product(activated, lax.all_gather(down_weight, "fs", axis=1, tiled=True))
    branch = lax.psum_scatter(partials, "tp", scatter_dimension=1, tiled=True)
    return (widened + branch).astype(jnp.bfloat16)


def dot_of(left, right):
    return jnp.dot(left, right, preferred_element_type=jnp.float32)


def first_projection_kernel(at, mixed, flip1, flip2, flip3, weight, piece, stacked, near, far):
    half = piece.shape[1]
    for flip, block in enumerate((mixed, flip1, flip2, flip3)):
        stacked[flip] = block[...]
    mine = weight[:, pl.ds(pl.multiple_of(at[4] * half, half), half)]
    other = weight[:, pl.ds(pl.multiple_of((1 - at[4]) * half, half), half)]
    near[...] = dot_of(stacked[at[0]], mine) + dot_of(stacked[at[1]], piece[...])
    far[...] = dot_of(stacked[at[0]], other)


def second_projection_kernel(at, stacked, piece, near, out):
    out[...] = near[...] + dot_of(stacked[at[3]], piece[...])


def third_projection_kernel(at, stacked, piece2, far1, far3, near, far, near_out, far_out):
    near_out[...] = near[...] + dot_of(stacked[at[2]], piece2[...])
    far_out[...] = far[...] + dot_of(stacked[at[1]], far1[...]) + dot_of(stacked[at[3]], far3[...])


def last_projection_kernel(at, stacked, far2, near, far, stream, gain, resid, scaled):
    half = far2.shape[1]
    other = far[...] + dot_of(stacked[at[2]], far2[...])
    for side, value in ((at[4], near[...]), (1 - at[4], other)):
        columns = pl.ds(pl.multiple_of(side * half, half), half)
        kept = (stream[:, columns].astype(jnp.float32) + value).astype(jnp.bfloat16)
        resid[:, columns] = kept
        scaled[:, columns] = (kept.astype(jnp.float32) * gain[:, columns].astype(jnp.float32)).astype(jnp.bfloat16)


def inverse_kernel(features, one, two, out):
    out[...] = 1.0 / ((one[...] + two[...]) / features + epsilon)


def hidden_kernel(place, own_a, pair_a, others_a, own_b, pair_b, others_b, *rest):
    near, far, out, weights = rest[:4], rest[4:6], rest[6], rest[7]
    depth, half = near[0].shape
    for slot, piece in enumerate(near):
        rows = pl.ds(pl.multiple_of(place[slot] * depth, depth), depth)
        weights[rows, :half] = piece[...]
        weights[rows, half:] = far[0][...] if slot == 0 else far[1][slot - 1]
    count = own_a.shape[0]
    for group, (own, pair, others) in enumerate(((own_a, pair_a, others_a), (own_b, pair_b, others_b))):
        total = jnp.zeros((count, 2 * half), jnp.float32)
        for flip, block in enumerate((own, others, pair, others)):
            left = block[flip // 2] if flip % 2 else block[...]
            total += jnp.dot(
                left, weights[flip * depth : (flip + 1) * depth, :], preferred_element_type=jnp.float32
            )
        out[group * count : (group + 1) * count, :] = jnp.square(jnp.maximum(total, 0.0)).astype(jnp.bfloat16)


def branch_products(hidden, weights, keep, give):
    for flip in (1, 3, 0, 2):
        value = jnp.dot(hidden, weights[flip], preferred_element_type=jnp.float32)
        target = give if flip % 2 else keep
        target[flip // 2] = value.astype(target.dtype)


def first_branch_kernel(count, place, hidden, *rest):
    near, far, keep, give, weights = rest[:4], rest[4:8], rest[8], rest[9], rest[10]
    half = near[0].shape[0]
    for slot in range(len(near)):
        weights[place[slot], :half, :] = near[slot][...]
        weights[place[slot], half:, :] = far[slot][...]
    branch_products(hidden[:count, :], weights, keep, give)


def second_branch_kernel(count, hidden, weights, keep, give):
    branch_products(hidden[count:, :], weights, keep, give)


def local_call(kernel, outs, *operands, flops, scratch=()):
    specs = [
        pl.BlockSpec(memory_space=pltpu.SMEM if x.dtype == jnp.int32 else pltpu.VMEM) for x in operands
    ]
    return pl.pallas_call(
        kernel,
        out_shape=outs,
        in_specs=specs,
        out_specs=jax.tree.map(lambda _: pl.BlockSpec(memory_space=pltpu.VMEM), outs),
        scratch_shapes=scratch,
        cost_estimate=pl.CostEstimate(flops=flops, bytes_accessed=1 << 20, transcendentals=0),
    )(*operands)


def gathered_tokens(parts, stream, mixed, out_weight, norm_gain, up_weight, down_weight):
    tokens, width = stream.shape
    half = width // 2
    unit = up_weight.shape[1] // parts
    part, row, column = lax.axis_index("grp"), lax.axis_index("fs"), lax.axis_index("tp")
    shifts = (1, 3, 2)

    def along_rows(value, shift):
        return lax.ppermute(value, "fs", [(i, (i + shift) % parts) for i in range(parts)])

    def across_parts(value):
        return lax.ppermute(value, "grp", [(0, 1), (1, 0)])

    def across_columns(value, flip):
        return lax.ppermute(value, "tp", [(i, i ^ flip) for i in range(parts)])

    def rows_at(value, begin, size):
        return lax.dynamic_slice_in_dim(value, begin, size, 0)

    def columns_at(value, begin, size):
        return lax.dynamic_slice_in_dim(value, begin, size, 1)

    at = jnp.stack([column ^ ((row - s) % parts) for s in range(parts)] + [part]).astype(jnp.int32)
    out_mine = columns_at(out_weight, part * half, half)
    out_near = {s: along_rows(out_mine, s) for s in shifts}
    flipped = [across_columns(mixed, flip) for flip in (1, 2, 3)]
    out_far = {s: across_parts(out_near[s]) for s in shifts}
    sums = jax.ShapeDtypeStruct((tokens, half), jnp.float32)
    flops = 2 * tokens * width * half
    stacked, near, far = local_call(
        first_projection_kernel,
        (jax.ShapeDtypeStruct((parts, tokens, width), jnp.bfloat16), sums, sums),
        at, mixed, *flipped, out_weight, out_near[1],
        flops=3 * flops,
    )
    near = local_call(second_projection_kernel, sums, at, stacked, out_near[3], near, flops=flops)
    near, far = local_call(
        third_projection_kernel, (sums, sums),
        at, stacked, out_near[2], out_far[1], out_far[3], near, far,
        flops=3 * flops,
    )
    resid, scaled = local_call(
        last_projection_kernel,
        (jax.ShapeDtypeStruct((tokens, width), jnp.bfloat16),) * 2,
        at, stacked, out_far[2], near, far, stream, norm_gain.reshape(1, width),
        flops=flops,
    )
    widened = resid.astype(jnp.float32)
    power = jnp.sum(widened * widened, axis=1).reshape(-1, 128)
    power += across_columns(power, 1)
    inverse = local_call(
        functools.partial(inverse_kernel, parts * width),
        jax.ShapeDtypeStruct(power.shape, jnp.float32),
        power, across_columns(power, 2),
        flops=1024,
    )

    def up_piece(s, side):
        return columns_at(up_weight, ((row + s) % parts) * unit + side * (unit // 2), unit // 2)

    def down_piece(s, side):
        return rows_at(down_weight, ((row + s) % parts) * unit + side * (unit // 2), unit // 2)

    up_near = {s: along_rows(up_piece(s, part), s) for s in shifts}
    up_far = across_parts(jnp.stack([up_near[s] for s in (1, 2, 3)]))
    down_near = {s: along_rows(down_piece(s, part), s) for s in shifts}
    down_far = {s: across_parts(down_near[s]) for s in shifts}
    place = jnp.stack([column ^ ((row - s) % parts) for s in range(parts)]).astype(jnp.int32)

    pairs = {0: across_columns(scaled, 2)}
    rows = {0: scaled} | {s: along_rows(scaled, s) for s in shifts}
    pairs[2] = across_columns(rows[2], 2)
    odd = jnp.concatenate([rows[1], rows[3]])
    even = jnp.concatenate([rows[0], rows[2]])
    even_pair = jnp.concatenate([pairs[0], pairs[2]])
    odd_pair = across_columns(odd, 2)
    even_others = across_columns(jnp.stack([even, even_pair]), 1)
    odd_others = across_columns(jnp.stack([odd, odd_pair]), 1)
    flops = 2 * parts * tokens * parts * width * unit
    hidden = local_call(
        hidden_kernel,
        jax.ShapeDtypeStruct((parts * tokens, unit), jnp.bfloat16),
        place, even, even_pair, even_others, odd, odd_pair, odd_others,
        up_piece(0, part), up_near[1], up_near[2], up_near[3], up_piece(0, 1 - part), up_far,
        flops=flops,
        scratch=[pltpu.VMEM((parts * width, unit), jnp.bfloat16)],
    )
    count = 2 * tokens
    halves = (
        jax.ShapeDtypeStruct((2, count, width), jnp.float32),
        jax.ShapeDtypeStruct((2, count, width), jnp.bfloat16),
    )
    keep_a, give_a, down_whole = local_call(
        functools.partial(first_branch_kernel, count),
        (*halves, jax.ShapeDtypeStruct((parts, unit, width), jnp.bfloat16)),
        place, hidden,
        down_piece(0, part), down_near[1], down_near[2], down_near[3],
        down_piece(0, 1 - part), down_far[1], down_far[2], down_far[3],
        flops=flops // 2,
    )
    keep_b, give_b = local_call(
        functools.partial(second_branch_kernel, count), halves, hidden, down_whole, flops=flops // 2
    )
    got_a = across_columns(give_a, 1)
    got_b = across_columns(give_b, 1)
    even_give = (keep_a[1] + got_a[1]).astype(jnp.bfloat16)
    odd_give = (keep_b[1] + got_b[1]).astype(jnp.bfloat16)
    even_keep, odd_keep = keep_a[0] + got_a[0], keep_b[0] + got_b[0]
    two = even_keep[tokens:] + across_columns(even_give[tokens:], 2)
    odd_sum = (odd_keep + across_columns(odd_give, 2)).astype(jnp.bfloat16)
    branch = even_keep[:tokens] + across_columns(even_give[:tokens], 2)
    branch += along_rows(two.astype(jnp.bfloat16), -2)
    branch += along_rows(odd_sum[:tokens], -1)
    branch += along_rows(odd_sum[tokens:], -3)
    return (widened + branch * inverse.reshape(tokens, 1)).astype(jnp.bfloat16)


def solution(mesh):
    shape = mesh.shape
    placed = (
        P(("grp", "fs"), "tp"),
        P(("grp", "fs"), "tp"),
        P("fs", "tp"),
        P("tp"),
        P("fs", "tp"),
        P("tp", "fs"),
    )

    cut = shape["grp"] == 2 and shape["fs"] == 4 and shape["tp"] == 4

    def body(*blocks):
        if not cut:
            return gathered_weights(*blocks)
        return gathered_tokens(shape["fs"], *blocks)

    return jax.shard_map(
        body, mesh=mesh, in_specs=placed, out_specs=P(("grp", "fs"), "tp"), check_vma=False
    )
```

```python
import functools

import jax
import jax.numpy as jnp
from jax import lax
from jax.experimental import pallas as pl
from jax.experimental.pallas import tpu as pltpu
from jax.sharding import PartitionSpec as P

epsilon = 1e-06


def fold_product(left, portion):
    return jnp.dot(left, portion, preferred_element_type=jnp.float32)


def gathered_weights(stream, mixed, out_weight, norm_gain, up_weight, down_weight):
    mixed_whole = lax.all_gather(mixed, "tp", axis=1, tiled=True)
    projected = fold_product(mixed_whole, lax.all_gather(out_weight, "fs", axis=0, tiled=True))
    resid = (stream.astype(jnp.float32) + projected).astype(jnp.bfloat16)
    widened = resid.astype(jnp.float32)
    resid_whole, gain_whole = (
        lax.all_gather(resid, "tp", axis=1, tiled=True),
        lax.all_gather(norm_gain, "tp", axis=0, tiled=True),
    )
    stream_wide = resid_whole.astype(jnp.float32)
    energy = jnp.mean(stream_wide * stream_wide, axis=1, keepdims=True)
    normed_whole = (
        stream_wide * lax.rsqrt(energy + epsilon) * gain_whole.astype(jnp.float32)
    ).astype(jnp.bfloat16)
    up_full = lax.all_gather(up_weight, "fs", axis=0, tiled=True)
    up_values = fold_product(normed_whole, up_full)
    activated = jnp.square(jax.nn.relu(up_values)).astype(jnp.bfloat16)
    partials = fold_product(activated, lax.all_gather(down_weight, "fs", axis=1, tiled=True))
    branch = lax.psum_scatter(partials, "tp", scatter_dimension=1, tiled=True)
    return (widened + branch).astype(jnp.bfloat16)


def dot_of(left, right):
    return jnp.dot(left, right, preferred_element_type=jnp.float32)


def first_projection_kernel(at, mixed, flip1, flip2, flip3, weight, piece, stacked, near, far):
    half = piece.shape[1]
    for flip, block in enumerate((mixed, flip1, flip2, flip3)):
        stacked[flip] = block[...]
    mine = weight[:, pl.ds(pl.multiple_of(at[4] * half, half), half)]
    other = weight[:, pl.ds(pl.multiple_of((1 - at[4]) * half, half), half)]
    near[...] = dot_of(stacked[at[0]], mine) + dot_of(stacked[at[1]], piece[...])
    far[...] = dot_of(stacked[at[0]], other)


def second_projection_kernel(at, stacked, piece, near, out):
    out[...] = near[...] + dot_of(stacked[at[3]], piece[...])


def third_projection_kernel(at, stacked, piece2, far1, far3, near, far, near_out, far_out):
    near_out[...] = near[...] + dot_of(stacked[at[2]], piece2[...])
    far_out[...] = far[...] + dot_of(stacked[at[1]], far1[...]) + dot_of(stacked[at[3]], far3[...])


def last_projection_kernel(at, stacked, far2, near, far, stream, gain, resid, scaled):
    half = far2.shape[1]
    other = far[...] + dot_of(stacked[at[2]], far2[...])
    for side, value in ((at[4], near[...]), (1 - at[4], other)):
        columns = pl.ds(pl.multiple_of(side * half, half), half)
        kept = (stream[:, columns].astype(jnp.float32) + value).astype(jnp.bfloat16)
        resid[:, columns] = kept
        scaled[:, columns] = (kept.astype(jnp.float32) * gain[:, columns].astype(jnp.float32)).astype(jnp.bfloat16)


def mean_kernel(features, one, two, out):
    out[...] = (one[...] + two[...]) / features


def inverse_kernel(energy, out):
    out[...] = 1.0 / (energy[...] + epsilon)


def hidden_products(own, pair, others, weights, out):
    depth = own.shape[1]
    total = None
    for flip, block in enumerate((own, others, pair, others)):
        left = block[flip // 2] if flip % 2 else block[...]
        term = dot_of(left, weights[flip * depth : (flip + 1) * depth, :])
        total = term if total is None else total + term
    out[...] = jnp.square(jnp.maximum(total, 0.0)).astype(jnp.bfloat16)


def first_hidden_kernel(place, own, pair, others, *rest):
    near, far, out, weights = rest[:4], rest[4:6], rest[6], rest[7]
    depth, half = near[0].shape
    for slot, piece in enumerate(near):
        rows = pl.ds(pl.multiple_of(place[slot] * depth, depth), depth)
        weights[rows, :half] = piece[...]
        weights[rows, half:] = far[0][...] if slot == 0 else far[1][slot - 1]
    hidden_products(own, pair, others, weights, out)


def second_hidden_kernel(own, pair, others, weights, out):
    hidden_products(own, pair, others, weights, out)


def branch_products(hidden, weights, keep, give):
    for flip in (1, 3, 0, 2):
        value = dot_of(hidden, weights[flip])
        target = give if flip % 2 else keep
        target[flip // 2] = value.astype(target.dtype)


def first_branch_kernel(place, hidden, *rest):
    near, far, keep, give, weights = rest[:4], rest[4:8], rest[8], rest[9], rest[10]
    half = near[0].shape[0]
    tokens = keep.shape[1]
    for slot in range(len(near)):
        weights[place[slot], :half, :] = near[slot][...]
        weights[place[slot], half:, :] = far[slot][...]
    branch_products(hidden[tokens:, :], weights, keep, give)


def second_branch_kernel(hidden, weights, keep, give):
    branch_products(hidden[...], weights, keep, give)


def third_branch_kernel(hidden, weights, keep, give):
    branch_products(hidden[: keep.shape[1], :], weights, keep, give)


def half_sum_kernel(keep, got, *outs):
    blocks = len(outs) // 2
    tokens = outs[0].shape[0]
    for block in range(blocks):
        rows = slice(block * tokens, (block + 1) * tokens)
        for side in range(2):
            out = outs[side * blocks + block]
            out[...] = (keep[side, rows, :] + got[side, rows, :].astype(jnp.float32)).astype(out.dtype)


def pair_sum_kernel(keep, got, out):
    out[...] = (keep[...] + got[...].astype(jnp.float32)).astype(out.dtype)


def local_call(kernel, outs, *operands, flops, scratch=(), room=8):
    specs = [
        pl.BlockSpec(memory_space=pltpu.SMEM if x.dtype == jnp.int32 else pltpu.VMEM) for x in operands
    ]
    return pl.pallas_call(
        kernel,
        out_shape=outs,
        in_specs=specs,
        out_specs=jax.tree.map(lambda _: pl.BlockSpec(memory_space=pltpu.VMEM), outs),
        scratch_shapes=scratch,
        compiler_params=pltpu.CompilerParams(vmem_limit_bytes=room << 20),
        cost_estimate=pl.CostEstimate(flops=flops, bytes_accessed=1 << 20, transcendentals=0),
    )(*operands)


def gathered_tokens(parts, stream, mixed, out_weight, norm_gain, up_weight, down_weight):
    tokens, width = stream.shape
    half = width // 2
    unit = up_weight.shape[1] // parts
    part, row, column = lax.axis_index("grp"), lax.axis_index("fs"), lax.axis_index("tp")
    shifts = (1, 3, 2)

    def along_rows(value, shift, around=True):
        moves = [(i, (i + shift) % parts) for i in range(parts)]
        if not around:
            moves = [(i, j) for i, j in moves if abs(i - j) < 3]
        return lax.ppermute(value, "fs", moves)

    def onward(value):
        return lax.ppermute(value, "fs", [(1, 0), (parts - 2, parts - 1)])

    def across_parts(value):
        return lax.ppermute(value, "grp", [(0, 1), (1, 0)])

    def across_columns(value, flip):
        return lax.ppermute(value, "tp", [(i, i ^ flip) for i in range(parts)])

    def rows_at(value, begin, size):
        return lax.dynamic_slice_in_dim(value, begin, size, 0)

    def columns_at(value, begin, size):
        return lax.dynamic_slice_in_dim(value, begin, size, 1)

    at = jnp.stack([column ^ ((row - s) % parts) for s in range(parts)] + [part]).astype(jnp.int32)
    out_mine = columns_at(out_weight, part * half, half)
    out_near = {s: along_rows(out_mine, s) for s in shifts}
    flipped = [across_columns(mixed, flip) for flip in (1, 2, 3)]
    out_far = {s: across_parts(out_near[s]) for s in shifts}
    sums = jax.ShapeDtypeStruct((tokens, half), jnp.float32)
    flops = 2 * tokens * width * half
    stacked, near, far = local_call(
        first_projection_kernel,
        (jax.ShapeDtypeStruct((parts, tokens, width), jnp.bfloat16), sums, sums),
        at, mixed, *flipped, out_weight, out_near[1],
        flops=3 * flops,
    )
    near = local_call(second_projection_kernel, sums, at, stacked, out_near[3], near, flops=flops)
    near, far = local_call(
        third_projection_kernel, (sums, sums),
        at, stacked, out_near[2], out_far[1], out_far[3], near, far,
        flops=3 * flops,
    )
    resid, scaled = local_call(
        last_projection_kernel,
        (jax.ShapeDtypeStruct((tokens, width), jnp.bfloat16),) * 2,
        at, stacked, out_far[2], near, far, stream, norm_gain.reshape(1, width),
        flops=flops,
    )
    widened = resid.astype(jnp.float32)
    power = jnp.sum(widened * widened, axis=1).reshape(-1, 128)
    power += across_columns(power, 1)
    small = jax.ShapeDtypeStruct(power.shape, jnp.float32)
    energy = local_call(
        functools.partial(mean_kernel, parts * width), small, power, across_columns(power, 2), flops=1024
    )
    inverse = local_call(inverse_kernel, small, energy, flops=1024)

    def up_piece(s, side):
        return columns_at(up_weight, ((row + s) % parts) * unit + side * (unit // 2), unit // 2)

    def down_piece(s, side):
        return rows_at(down_weight, ((row + s) % parts) * unit + side * (unit // 2), unit // 2)

    up_near = {s: along_rows(up_piece(s, part), s) for s in shifts}
    up_far = across_parts(jnp.stack([up_near[s] for s in (1, 2, 3)]))
    down_near = {s: along_rows(down_piece(s, part), s) for s in shifts}
    down_far = {s: across_parts(down_near[s]) for s in shifts}
    place = jnp.stack([column ^ ((row - s) % parts) for s in range(parts)]).astype(jnp.int32)

    pairs = {0: across_columns(scaled, 2)}
    rows = {0: scaled} | {s: along_rows(scaled, s, around=False) for s in shifts}
    end = onward(rows[2])
    rows[1] = jnp.where(row == 0, end, rows[1])
    rows[3] = jnp.where(row == parts - 1, end, rows[3])
    pairs[2] = across_columns(rows[2], 2)
    odd = jnp.concatenate([rows[1], rows[3]])
    even = jnp.concatenate([rows[0], rows[2]])
    even_pair = jnp.concatenate([pairs[0], pairs[2]])
    odd_pair = across_columns(odd, 2)
    even_both = jnp.stack([even, even_pair])
    even_others = across_columns(even_both, 1)
    odd_others = across_columns(jnp.stack([odd, odd_pair]), 1)
    flops = 4 * tokens * parts * width * unit
    some = jax.ShapeDtypeStruct((2 * tokens, unit), jnp.bfloat16)
    hidden_even, up_whole = local_call(
        first_hidden_kernel,
        (some, jax.ShapeDtypeStruct((parts * width, unit), jnp.bfloat16)),
        place, even, even_pair, even_others,
        up_piece(0, part), up_near[1], up_near[2], up_near[3], up_piece(0, 1 - part), up_far,
        flops=flops,
        room=14,
    )
    hidden_odd = local_call(second_hidden_kernel, some, odd, odd_pair, odd_others, up_whole, flops=flops, room=14)

    def halves(count):
        shape = (2, count, width)
        return jax.ShapeDtypeStruct(shape, jnp.float32), jax.ShapeDtypeStruct(shape, jnp.bfloat16)

    keep_two, give_two, down_whole = local_call(
        first_branch_kernel,
        (*halves(tokens), jax.ShapeDtypeStruct((parts, unit, width), jnp.bfloat16)),
        place, hidden_even,
        down_piece(0, part), down_near[1], down_near[2], down_near[3],
        down_piece(0, 1 - part), down_far[1], down_far[2], down_far[3],
        flops=flops // 2,
        room=14,
    )
    keep_odd, give_odd = local_call(
        second_branch_kernel, halves(2 * tokens), hidden_odd, down_whole, flops=flops, room=14
    )
    keep_own, give_own = local_call(
        third_branch_kernel, halves(tokens), hidden_even, down_whole, flops=flops // 2, room=14
    )

    block = (tokens, width)

    def halved(keep, give):
        blocks = keep.shape[1] // tokens
        outs = [jax.ShapeDtypeStruct(block, kind) for kind in (jnp.float32, jnp.bfloat16) for _ in range(blocks)]
        return local_call(half_sum_kernel, outs, keep, across_columns(give, 1), flops=1024)

    def summed(keep, give):
        out = jax.ShapeDtypeStruct(block, jnp.bfloat16)
        return local_call(pair_sum_kernel, out, keep, across_columns(give, 2), flops=1024)

    keep_two, give_two = halved(keep_two, give_two)
    keep_one, keep_three, give_one, give_three = halved(keep_odd, give_odd)
    keep_own, give_own = halved(keep_own, give_own)
    two = summed(keep_two, give_two)
    one = summed(keep_one, give_one)
    three = summed(keep_three, give_three)
    branch = keep_own + across_columns(give_own, 2)
    branch += along_rows(two, -2)
    branch += along_rows(one, -1)
    branch += along_rows(three, -3)
    return (widened + branch * inverse.reshape(tokens, 1)).astype(jnp.bfloat16)


def solution(mesh):
    shape = mesh.shape
    placed = (
        P(("grp", "fs"), "tp"),
        P(("grp", "fs"), "tp"),
        P("fs", "tp"),
        P("tp"),
        P("fs", "tp"),
        P("tp", "fs"),
    )

    cut = shape["grp"] == 2 and shape["fs"] == 4 and shape["tp"] == 4

    def body(*blocks):
        if not cut:
            return gathered_weights(*blocks)
        return gathered_tokens(shape["fs"], *blocks)

    return jax.shard_map(
        body, mesh=mesh, in_specs=placed, out_specs=P(("grp", "fs"), "tp"), check_vma=False
    )
```

```python
import functools

import jax
import jax.numpy as jnp
from jax import lax
from jax.experimental import pallas as pl
from jax.experimental.pallas import tpu as pltpu
from jax.sharding import PartitionSpec as P

epsilon = 1e-06


def fold_product(left, portion):
    return jnp.dot(left, portion, preferred_element_type=jnp.float32)


def gathered_weights(stream, mixed, out_weight, norm_gain, up_weight, down_weight):
    mixed_whole = lax.all_gather(mixed, "tp", axis=1, tiled=True)
    projected = fold_product(mixed_whole, lax.all_gather(out_weight, "fs", axis=0, tiled=True))
    resid = (stream.astype(jnp.float32) + projected).astype(jnp.bfloat16)
    widened = resid.astype(jnp.float32)
    resid_whole, gain_whole = (
        lax.all_gather(resid, "tp", axis=1, tiled=True),
        lax.all_gather(norm_gain, "tp", axis=0, tiled=True),
    )
    stream_wide = resid_whole.astype(jnp.float32)
    energy = jnp.mean(stream_wide * stream_wide, axis=1, keepdims=True)
    normed_whole = (
        stream_wide * lax.rsqrt(energy + epsilon) * gain_whole.astype(jnp.float32)
    ).astype(jnp.bfloat16)
    up_full = lax.all_gather(up_weight, "fs", axis=0, tiled=True)
    up_values = fold_product(normed_whole, up_full)
    activated = jnp.square(jax.nn.relu(up_values)).astype(jnp.bfloat16)
    partials = fold_product(activated, lax.all_gather(down_weight, "fs", axis=1, tiled=True))
    branch = lax.psum_scatter(partials, "tp", scatter_dimension=1, tiled=True)
    return (widened + branch).astype(jnp.bfloat16)


def dot_of(left, right):
    return jnp.dot(left, right, preferred_element_type=jnp.float32)


def first_projection_kernel(at, stacked, weight, near1, near2, near, far):
    half = near1.shape[1]
    mine = weight[:, pl.ds(pl.multiple_of(at[4] * half, half), half)]
    other = weight[:, pl.ds(pl.multiple_of((1 - at[4]) * half, half), half)]
    near[...] = (
        dot_of(stacked[at[0]], mine) + dot_of(stacked[at[1]], near1[...]) + dot_of(stacked[at[2]], near2[...])
    )
    far[...] = dot_of(stacked[at[0]], other)


def second_projection_kernel(at, stacked, near3, far1, far2, near, far, near_out, far_out):
    near_out[...] = near[...] + dot_of(stacked[at[3]], near3[...])
    far_out[...] = far[...] + dot_of(stacked[at[1]], far1[...]) + dot_of(stacked[at[2]], far2[...])


def last_projection_kernel(at, stacked, far3, near, far, stream, gain, resid, scaled):
    half = far3.shape[1]
    other = far[...] + dot_of(stacked[at[3]], far3[...])
    for side, value in ((at[4], near[...]), (1 - at[4], other)):
        columns = pl.ds(pl.multiple_of(side * half, half), half)
        kept = (stream[:, columns].astype(jnp.float32) + value).astype(jnp.bfloat16)
        resid[:, columns] = kept
        scaled[:, columns] = (kept.astype(jnp.float32) * gain[:, columns].astype(jnp.float32)).astype(jnp.bfloat16)


def mean_kernel(features, one, two, out):
    out[...] = (one[...] + two[...]) / features


def inverse_kernel(energy, out):
    out[...] = 1.0 / (energy[...] + epsilon)


def hidden_products(own, pair, others, weights, out):
    depth = own.shape[1]
    total = None
    for flip, block in enumerate((own, others, pair, others)):
        left = block[flip // 2] if flip % 2 else block[...]
        term = dot_of(left, weights[flip * depth : (flip + 1) * depth, :])
        total = term if total is None else total + term
    out[...] = jnp.square(jnp.maximum(total, 0.0)).astype(jnp.bfloat16)


def first_hidden_kernel(place, own, pair, others, *rest):
    near, far, out, weights = rest[:4], rest[4:6], rest[6], rest[7]
    depth, half = near[0].shape
    for slot, piece in enumerate(near):
        rows = pl.ds(pl.multiple_of(place[slot] * depth, depth), depth)
        weights[rows, :half] = piece[...]
        weights[rows, half:] = far[0][...] if slot == 0 else far[1][slot - 1]
    hidden_products(own, pair, others, weights, out)


def second_hidden_kernel(own, pair, others, weights, out):
    hidden_products(own, pair, others, weights, out)


def branch_products(own, other, weights, keep, give):
    depth = own.shape[1]
    for side, target in ((1, give), (0, keep)):
        value = dot_of(own, weights[side, :depth, :]) + dot_of(other, weights[side, depth:, :])
        target[...] = value.astype(target.dtype)


def first_branch_kernel(place, own, other, *rest):
    near, far, keep, give, weights = rest[:4], rest[4:8], rest[8], rest[9], rest[10]
    half = near[0].shape[0]
    tokens = keep.shape[0]
    for slot in range(len(near)):
        begin = pl.multiple_of(place[len(near) + slot] * (2 * half), 2 * half)
        weights[place[slot], pl.ds(begin, half), :] = near[slot][...]
        weights[place[slot], pl.ds(begin + half, half), :] = far[slot][...]
    branch_products(own[tokens:, :], other[tokens:, :], weights, keep, give)


def second_branch_kernel(own, other, weights, keep_one, give_one, keep_three, give_three):
    tokens = keep_one.shape[0]
    branch_products(own[:tokens, :], other[:tokens, :], weights, keep_one, give_one)
    branch_products(own[tokens:, :], other[tokens:, :], weights, keep_three, give_three)


def third_branch_kernel(own, other, weights, keep, give):
    tokens = keep.shape[0]
    branch_products(own[:tokens, :], other[:tokens, :], weights, keep, give)


def pair_sum_kernel(keep, got, out):
    out[...] = (keep[...] + got[...].astype(jnp.float32)).astype(out.dtype)


def cut_kernel(axis, at, whole, *rest):
    outs, sems = rest[:-1], rest[-1]
    copies = []
    for number, out in enumerate(outs):
        size = out.shape[axis]
        span = pl.ds(pl.multiple_of(at[number] * size, size), size)
        source = whole.at[span, :] if axis == 0 else whole.at[:, span]
        copies.append(pltpu.make_async_copy(source, out, sems.at[number]))
        copies[-1].start()
    for copy in copies:
        copy.wait()


def cut(whole, axis, size, starts):
    shape = tuple(size if i == axis else n for i, n in enumerate(whole.shape))
    out = jax.ShapeDtypeStruct(shape, whole.dtype)
    place = jnp.stack([jnp.asarray(x, jnp.int32) for x in starts])
    return pl.pallas_call(
        functools.partial(cut_kernel, axis),
        out_shape=[out] * len(starts),
        in_specs=[pl.BlockSpec(memory_space=pltpu.SMEM), pl.BlockSpec(memory_space=pltpu.HBM)],
        out_specs=[pl.BlockSpec(memory_space=pltpu.VMEM)] * len(starts),
        scratch_shapes=[pltpu.SemaphoreType.DMA((len(starts),))],
        compiler_params=pltpu.CompilerParams(vmem_limit_bytes=4 << 20),
        cost_estimate=pl.CostEstimate(flops=1024, bytes_accessed=1 << 20, transcendentals=0),
    )(place, whole)


def local_call(kernel, outs, *operands, flops, scratch=(), room=8):
    specs = [
        pl.BlockSpec(memory_space=pltpu.SMEM if x.dtype == jnp.int32 else pltpu.VMEM) for x in operands
    ]
    return pl.pallas_call(
        kernel,
        out_shape=outs,
        in_specs=specs,
        out_specs=jax.tree.map(lambda _: pl.BlockSpec(memory_space=pltpu.VMEM), outs),
        scratch_shapes=scratch,
        compiler_params=pltpu.CompilerParams(vmem_limit_bytes=room << 20),
        cost_estimate=pl.CostEstimate(flops=flops, bytes_accessed=1 << 20, transcendentals=0),
    )(*operands)


def gathered_tokens(parts, stream, mixed, out_weight, norm_gain, up_weight, down_weight):
    tokens, width = stream.shape
    half = width // 2
    unit = up_weight.shape[1] // parts
    part, row, column = lax.axis_index("grp"), lax.axis_index("fs"), lax.axis_index("tp")
    flips = (1, 2, 3)

    def along_rows(value, flip):
        return lax.ppermute(value, "fs", [(i, i ^ flip) for i in range(parts)])

    def across_parts(value):
        return lax.ppermute(value, "grp", [(0, 1), (1, 0)])

    def across_columns(value, flip):
        return lax.ppermute(value, "tp", [(i, i ^ flip) for i in range(parts)])

    at = jnp.stack([column ^ row ^ s for s in range(parts)] + [part]).astype(jnp.int32)
    (out_mine,) = cut(out_weight, 1, half, [part])
    out_near = {s: along_rows(out_mine, s) for s in (1, 2)}
    out_near[3] = along_rows(out_near[2], 1)
    flipped = [across_columns(mixed, flip) for flip in (1, 2, 3)]
    out_far = {s: across_parts(out_near[s]) for s in flips}
    sums = jax.ShapeDtypeStruct((tokens, half), jnp.float32)
    flops = 2 * tokens * width * half
    stacked = jnp.stack([mixed, *flipped])
    near, far = local_call(
        first_projection_kernel, (sums, sums), at, stacked, out_weight, out_near[1], out_near[2], flops=3 * flops
    )
    near, far = local_call(
        second_projection_kernel, (sums, sums),
        at, stacked, out_near[3], out_far[1], out_far[2], near, far,
        flops=3 * flops,
    )
    resid, scaled = local_call(
        last_projection_kernel,
        (jax.ShapeDtypeStruct((tokens, width), jnp.bfloat16),) * 2,
        at, stacked, out_far[3], near, far, stream, norm_gain.reshape(1, width),
        flops=flops,
    )
    widened = resid.astype(jnp.float32)
    power = jnp.sum(widened * widened, axis=1).reshape(-1, 128)
    power += across_columns(power, 1)
    small = jax.ShapeDtypeStruct(power.shape, jnp.float32)
    energy = local_call(
        functools.partial(mean_kernel, parts * width), small, power, across_columns(power, 2), flops=1024
    )
    inverse = local_call(inverse_kernel, small, energy, flops=1024)

    wanted = [2 * (row ^ s) + part for s in (0, *flips)] + [2 * row + 1 - part]
    up_mine, *up_sent, up_other = cut(up_weight, 1, unit // 2, wanted)
    up_near = {s: along_rows(piece, s) for s, piece in zip(flips, up_sent)}
    up_far = across_parts(jnp.stack([up_near[s] for s in (1, 2, 3)]))
    core = column % 2
    odd_one = (row ^ core) % 2
    down_near, down_far, sides, sources = [], [], [], []
    turns = ((0, 0), (0, 1), (2, 0), (2, 1))
    wanted = [2 * (row ^ (pair + (core ^ turn))) + part for pair, turn in turns]
    down_sent = cut(down_weight, 0, unit // 2, wanted)
    for number, (pair, turn) in enumerate(turns):
        moves = []
        for i in range(parts):
            for j in range(parts):
                moves.append((i * parts + j, (i ^ (pair + (j % 2 ^ turn))) * parts + j // 2 * 2 + i % 2))
        down_near.append(lax.ppermute(down_sent[number], ("fs", "tp"), moves))
        down_far.append(across_parts(down_near[-1]))
        sides.append(((row ^ (pair + odd_one)) != column).astype(jnp.int32))
        sources.append((odd_one ^ turn ^ core).astype(jnp.int32))
    down_place = jnp.stack(sides + sources)
    place = at[:parts]

    pairs = {0: across_columns(scaled, 2)}
    rows = {s: along_rows(scaled, s) for s in (1, 2)}
    rows[3] = along_rows(rows[2], 1)
    pairs |= {s: across_columns(rows[s], 2) for s in flips}
    even = jnp.concatenate([scaled, rows[2]])
    odd = jnp.concatenate([rows[1], rows[3]])
    even_pair = jnp.concatenate([pairs[0], pairs[2]])
    odd_pair = jnp.concatenate([pairs[1], pairs[3]])
    even_both = jnp.stack([even, even_pair])
    even_others = across_columns(even_both, 1)
    odd_others = across_columns(jnp.stack([odd, odd_pair]), 1)
    flops = 4 * tokens * parts * width * unit
    some = jax.ShapeDtypeStruct((2 * tokens, unit), jnp.bfloat16)
    hidden_even, up_whole = local_call(
        first_hidden_kernel,
        (some, jax.ShapeDtypeStruct((parts * width, unit), jnp.bfloat16)),
        place, even, even_pair, even_others,
        up_mine, up_near[1], up_near[2], up_near[3], up_other, up_far,
        flops=flops,
        room=14,
    )
    hidden_odd = local_call(second_hidden_kernel, some, odd, odd_pair, odd_others, up_whole, flops=flops, room=14)

    block = (tokens, width)
    pair_of = (jax.ShapeDtypeStruct(block, jnp.float32), jax.ShapeDtypeStruct(block, jnp.bfloat16))
    other_even = across_columns(hidden_even, 1)
    other_odd = across_columns(hidden_odd, 1)
    keep_two, give_two, down_whole = local_call(
        first_branch_kernel,
        (*pair_of, jax.ShapeDtypeStruct((2, 2 * unit, width), jnp.bfloat16)),
        down_place, hidden_even, other_even, *down_near, *down_far,
        flops=flops // 2,
        room=14,
    )
    keep_one, give_one, keep_three, give_three = local_call(
        second_branch_kernel, pair_of * 2, hidden_odd, other_odd, down_whole, flops=flops, room=14
    )
    keep_own, give_own = local_call(
        third_branch_kernel, pair_of, hidden_even, other_even, down_whole, flops=flops // 2, room=14
    )

    def summed(keep, give):
        out = jax.ShapeDtypeStruct(block, jnp.bfloat16)
        return local_call(pair_sum_kernel, out, keep, across_columns(give, 2), flops=1024)

    two = summed(keep_two, give_two)
    one = summed(keep_one, give_one)
    three = summed(keep_three, give_three)
    branch = keep_own + across_columns(give_own, 2)
    branch += along_rows(two, 2)
    branch += along_rows(one, 1)
    branch += along_rows(three, 3)
    return (widened + branch * inverse.reshape(tokens, 1)).astype(jnp.bfloat16)


def solution(mesh):
    shape = mesh.shape
    placed = (
        P(("grp", "fs"), "tp"),
        P(("grp", "fs"), "tp"),
        P("fs", "tp"),
        P("tp"),
        P("fs", "tp"),
        P("tp", "fs"),
    )

    cut = shape["grp"] == 2 and shape["fs"] == 4 and shape["tp"] == 4

    def body(*blocks):
        if not cut:
            return gathered_weights(*blocks)
        return gathered_tokens(shape["fs"], *blocks)

    return jax.shard_map(
        body, mesh=mesh, in_specs=placed, out_specs=P(("grp", "fs"), "tp"), check_vma=False
    )
```

```python
import functools

import jax
import jax.numpy as jnp
from jax import lax
from jax.experimental import pallas as pl
from jax.experimental.pallas import tpu as pltpu
from jax.sharding import PartitionSpec as P

epsilon = 1e-06


def fold_product(left, portion):
    return jnp.dot(left, portion, preferred_element_type=jnp.float32)


def gathered_weights(stream, mixed, out_weight, norm_gain, up_weight, down_weight):
    mixed_whole = lax.all_gather(mixed, "tp", axis=1, tiled=True)
    projected = fold_product(mixed_whole, lax.all_gather(out_weight, "fs", axis=0, tiled=True))
    resid = (stream.astype(jnp.float32) + projected).astype(jnp.bfloat16)
    widened = resid.astype(jnp.float32)
    resid_whole, gain_whole = (
        lax.all_gather(resid, "tp", axis=1, tiled=True),
        lax.all_gather(norm_gain, "tp", axis=0, tiled=True),
    )
    stream_wide = resid_whole.astype(jnp.float32)
    energy = jnp.mean(stream_wide * stream_wide, axis=1, keepdims=True)
    normed_whole = (
        stream_wide * lax.rsqrt(energy + epsilon) * gain_whole.astype(jnp.float32)
    ).astype(jnp.bfloat16)
    up_full = lax.all_gather(up_weight, "fs", axis=0, tiled=True)
    up_values = fold_product(normed_whole, up_full)
    activated = jnp.square(jax.nn.relu(up_values)).astype(jnp.bfloat16)
    partials = fold_product(activated, lax.all_gather(down_weight, "fs", axis=1, tiled=True))
    branch = lax.psum_scatter(partials, "tp", scatter_dimension=1, tiled=True)
    return (widened + branch).astype(jnp.bfloat16)


def dot_of(left, right):
    return jnp.dot(left, right, preferred_element_type=jnp.float32)


def most_projection_kernel(at, stacked, weight, near1, near2, near3, far1, far2, stream, near, far):
    half = near1.shape[1]
    mine = pl.ds(pl.multiple_of(at[4] * half, half), half)
    other = pl.ds(pl.multiple_of((1 - at[4]) * half, half), half)
    total = dot_of(stacked[at[0]], weight[:, mine])
    for flip, piece in ((1, near1), (2, near2), (3, near3)):
        total += dot_of(stacked[at[flip]], piece[...])
    near[...] = stream[:, mine].astype(jnp.float32) + total
    total = dot_of(stacked[at[0]], weight[:, other])
    for flip, piece in ((1, far1), (2, far2)):
        total += dot_of(stacked[at[flip]], piece[...])
    far[...] = stream[:, other].astype(jnp.float32) + total


def last_projection_kernel(at, stacked, far3, near, far, gain, resid, scaled):
    half = far3.shape[1]
    last = far[...] + dot_of(stacked[at[3]], far3[...])
    for side, value in ((at[4], near[...]), (1 - at[4], last)):
        columns = pl.ds(pl.multiple_of(side * half, half), half)
        kept = value.astype(jnp.bfloat16)
        resid[:, columns] = kept
        scaled[:, columns] = (kept.astype(jnp.float32) * gain[:, columns].astype(jnp.float32)).astype(jnp.bfloat16)


def stack_kernel(own_first, own_second, pair_first, pair_second, out):
    tokens = own_first.shape[0]
    for side, blocks in enumerate(((own_first, own_second), (pair_first, pair_second))):
        for number, block in enumerate(blocks):
            out[side, number * tokens : (number + 1) * tokens, :] = block[...]


def mean_kernel(features, one, two, out):
    out[...] = (one[...] + two[...]) / features


def inverse_kernel(energy, out):
    out[...] = 1.0 / (energy[...] + epsilon)


def hidden_products(mine, others, weights, out):
    depth = mine.shape[2]
    total = None
    for flip in range(4):
        left = (others if flip % 2 else mine)[flip // 2]
        term = dot_of(left, weights[flip * depth : (flip + 1) * depth, :])
        total = term if total is None else total + term
    out[...] = jnp.square(jnp.maximum(total, 0.0)).astype(jnp.bfloat16)


def first_hidden_kernel(place, mine, others, *rest):
    near, far, out, weights = rest[:4], rest[4:6], rest[6], rest[7]
    depth, half = near[0].shape
    for slot, piece in enumerate(near):
        rows = pl.ds(pl.multiple_of(place[slot] * depth, depth), depth)
        weights[rows, :half] = piece[...]
        weights[rows, half:] = far[0][...] if slot == 0 else far[1][slot - 1]
    hidden_products(mine, others, weights, out)


def second_hidden_kernel(mine, others, weights, out):
    hidden_products(mine, others, weights, out)


def branch_products(place, own, other, last, weights, keep, give):
    depth = own.shape[1]
    half = last.shape[0]
    extra = dot_of(jnp.where(place[7] == 0, own[:, half:], other[:, half:]), last[...])
    for side, target in ((1, give), (0, keep)):
        value = dot_of(own, weights[side, :depth, :]) + dot_of(other, weights[side, depth:, :])
        value += jnp.where(place[3] == side, extra, 0.0)
        target[...] = value.astype(target.dtype)


def place_piece(place, weights, slot, far, piece):
    half = piece.shape[0]
    begin = pl.multiple_of(place[4 + slot] * (2 * half) + far * half, half)
    weights[place[slot], pl.ds(begin, half), :] = piece


def place_kernel(place, *rest):
    near, far, weights = rest[:4], rest[4:7], rest[7]
    for side, pieces in enumerate((near, far)):
        for slot, piece in enumerate(pieces):
            place_piece(place, weights, slot, side, piece[...])
    place_piece(place, weights, 3, 1, jnp.zeros_like(near[3]))


def later_branch_kernel(place, own, other, last, weights, keep, give):
    tokens = keep.shape[0]
    branch_products(place, own[tokens:, :], other[tokens:, :], last, weights, keep, give)


def both_branch_kernel(place, own, other, last, weights, keep_one, give_one, keep_three, give_three):
    tokens = keep_one.shape[0]
    branch_products(place, own[:tokens, :], other[:tokens, :], last, weights, keep_one, give_one)
    branch_products(place, own[tokens:, :], other[tokens:, :], last, weights, keep_three, give_three)


def first_branch_kernel(place, own, other, last, weights, keep, give):
    tokens = keep.shape[0]
    branch_products(place, own[:tokens, :], other[:tokens, :], last, weights, keep, give)


def pair_sum_kernel(keep, got, out):
    out[...] = (keep[...] + got[...].astype(jnp.float32)).astype(out.dtype)


def cut_kernel(axis, at, whole, *rest):
    outs, sems = rest[:-1], rest[-1]
    copies = []
    for number, out in enumerate(outs):
        size = out.shape[axis]
        span = pl.ds(pl.multiple_of(at[number] * size, size), size)
        source = whole.at[span, :] if axis == 0 else whole.at[:, span]
        copies.append(pltpu.make_async_copy(source, out, sems.at[number]))
        copies[-1].start()
    for copy in copies:
        copy.wait()


def cut(whole, axis, size, starts):
    shape = tuple(size if i == axis else n for i, n in enumerate(whole.shape))
    out = jax.ShapeDtypeStruct(shape, whole.dtype)
    place = jnp.stack([jnp.asarray(x, jnp.int32) for x in starts])
    return pl.pallas_call(
        functools.partial(cut_kernel, axis),
        out_shape=[out] * len(starts),
        in_specs=[pl.BlockSpec(memory_space=pltpu.SMEM), pl.BlockSpec(memory_space=pltpu.HBM)],
        out_specs=[pl.BlockSpec(memory_space=pltpu.VMEM)] * len(starts),
        scratch_shapes=[pltpu.SemaphoreType.DMA((len(starts),))],
        compiler_params=pltpu.CompilerParams(vmem_limit_bytes=4 << 20),
        cost_estimate=pl.CostEstimate(flops=1024, bytes_accessed=1 << 20, transcendentals=0),
    )(place, whole)


def local_call(kernel, outs, *operands, flops, room=8):
    specs = [
        pl.BlockSpec(memory_space=pltpu.SMEM if x.dtype == jnp.int32 else pltpu.VMEM) for x in operands
    ]
    return pl.pallas_call(
        kernel,
        out_shape=outs,
        in_specs=specs,
        out_specs=jax.tree.map(lambda _: pl.BlockSpec(memory_space=pltpu.VMEM), outs),
        compiler_params=pltpu.CompilerParams(vmem_limit_bytes=room << 20),
        cost_estimate=pl.CostEstimate(flops=flops, bytes_accessed=1 << 20, transcendentals=0),
    )(*operands)


def gathered_tokens(parts, stream, mixed, out_weight, norm_gain, up_weight, down_weight):
    tokens, width = stream.shape
    half = width // 2
    unit = up_weight.shape[1] // parts
    part, row, column = lax.axis_index("grp"), lax.axis_index("fs"), lax.axis_index("tp")
    flips = (1, 2, 3)

    def along_rows(value, flip):
        return lax.ppermute(value, "fs", [(i, i ^ flip) for i in range(parts)])

    def across_parts(value):
        return lax.ppermute(value, "grp", [(0, 1), (1, 0)])

    def across_columns(value, flip):
        return lax.ppermute(value, "tp", [(i, i ^ flip) for i in range(parts)])

    at = jnp.stack([column ^ row ^ s for s in range(parts)] + [part]).astype(jnp.int32)
    (out_mine,) = cut(out_weight, 1, half, [part])
    out_near = {s: along_rows(out_mine, s) for s in (1, 2)}
    out_near[3] = along_rows(out_near[2], 1)
    flipped = [across_columns(mixed, flip) for flip in (1, 2, 3)]
    out_far = {s: across_parts(out_near[s]) for s in flips}
    sums = jax.ShapeDtypeStruct((tokens, half), jnp.float32)
    flops = 2 * tokens * width * half
    stacked = jnp.stack([mixed, *flipped])
    near, far = local_call(
        most_projection_kernel, (sums, sums),
        at, stacked, out_weight, *(out_near[s] for s in flips), out_far[1], out_far[2], stream,
        flops=7 * flops,
    )
    resid, scaled = local_call(
        last_projection_kernel,
        (jax.ShapeDtypeStruct((tokens, width), jnp.bfloat16),) * 2,
        at, stacked, out_far[3], near, far, norm_gain.reshape(1, width),
        flops=flops,
    )
    widened = resid.astype(jnp.float32)
    power = jnp.sum(widened * widened, axis=1).reshape(-1, 128)
    power += across_columns(power, 2)
    small = jax.ShapeDtypeStruct(power.shape, jnp.float32)
    energy = local_call(
        functools.partial(mean_kernel, parts * width), small, power, across_columns(power, 1), flops=1024
    )
    inverse = local_call(inverse_kernel, small, energy, flops=1024)

    wanted = [2 * (row ^ s) + part for s in (0, *flips)] + [2 * row + 1 - part]
    up_mine, *up_sent, up_other = cut(up_weight, 1, unit // 2, wanted)
    up_near = {s: along_rows(piece, s) for s, piece in zip(flips, up_sent)}
    up_far = across_parts(jnp.stack([up_near[s] for s in (1, 2, 3)]))
    core = column % 2
    odd_one = (row ^ core) % 2
    down_near, down_far, sides, sources = [], [], [], []
    turns = ((0, 0), (0, 1), (2, 0), (2, 1))
    wanted = [2 * (row ^ (pair + (core ^ turn))) + part for pair, turn in turns]
    down_sent = cut(down_weight, 0, unit // 2, wanted)
    for number, (pair, turn) in enumerate(turns):
        moves = []
        for i in range(parts):
            for j in range(parts):
                moves.append((i * parts + j, (i ^ (pair + (j % 2 ^ turn))) * parts + j // 2 * 2 + i % 2))
        down_near.append(lax.ppermute(down_sent[number], ("fs", "tp"), moves))
        down_far.append(across_parts(down_near[-1]))
        sides.append(((row ^ (pair + odd_one)) != column).astype(jnp.int32))
        sources.append((odd_one ^ turn ^ core).astype(jnp.int32))
    down_place = jnp.stack(sides + sources)
    place = at[:parts]

    pairs = {0: across_columns(scaled, 2)}
    rows = {s: along_rows(scaled, s) for s in (1, 2)}
    rows[3] = along_rows(rows[2], 1)
    pairs |= {s: across_columns(rows[s], 2) for s in flips}
    both = jax.ShapeDtypeStruct((2, 2 * tokens, width), jnp.bfloat16)
    even = local_call(stack_kernel, both, scaled, rows[2], pairs[0], pairs[2], flops=1024)
    odd = local_call(stack_kernel, both, rows[1], rows[3], pairs[1], pairs[3], flops=1024)
    even_others = across_columns(even, 1)
    odd_others = across_columns(odd, 1)
    flops = 4 * tokens * parts * width * unit
    some = jax.ShapeDtypeStruct((2 * tokens, unit), jnp.bfloat16)
    hidden_even, up_whole = local_call(
        first_hidden_kernel,
        (some, jax.ShapeDtypeStruct((parts * width, unit), jnp.bfloat16)),
        place, even, even_others,
        up_mine, up_near[1], up_near[2], up_near[3], up_other, up_far,
        flops=flops,
        room=14,
    )
    hidden_odd = local_call(second_hidden_kernel, some, odd, odd_others, up_whole, flops=flops, room=14)

    block = (tokens, width)
    pair_of = (jax.ShapeDtypeStruct(block, jnp.float32), jax.ShapeDtypeStruct(block, jnp.bfloat16))
    other_even = across_columns(hidden_even, 1)
    other_odd = across_columns(hidden_odd, 1)
    whole = jax.ShapeDtypeStruct((2, 2 * unit, width), jnp.bfloat16)
    down_most = local_call(place_kernel, whole, down_place, *down_near, *down_far[:3], flops=1024, room=14)
    keep_two, give_two = local_call(
        later_branch_kernel, pair_of,
        down_place, hidden_even, other_even, down_far[3], down_most,
        flops=flops // 2, room=14,
    )
    keep_one, give_one, keep_three, give_three = local_call(
        both_branch_kernel, pair_of * 2,
        down_place, hidden_odd, other_odd, down_far[3], down_most,
        flops=flops, room=14,
    )
    keep_own, give_own = local_call(
        first_branch_kernel, pair_of,
        down_place, hidden_even, other_even, down_far[3], down_most,
        flops=flops // 2, room=14,
    )

    def summed(keep, give):
        out = jax.ShapeDtypeStruct(block, jnp.bfloat16)
        return local_call(pair_sum_kernel, out, keep, across_columns(give, 2), flops=1024)

    two = summed(keep_two, give_two)
    one = summed(keep_one, give_one)
    three = summed(keep_three, give_three)
    branch = keep_own + across_columns(give_own, 2)
    branch += along_rows(two, 2)
    branch += along_rows(one, 1)
    branch += along_rows(three, 3)
    return (widened + branch * inverse.reshape(tokens, 1)).astype(jnp.bfloat16)


def solution(mesh):
    shape = mesh.shape
    placed = (
        P(("grp", "fs"), "tp"),
        P(("grp", "fs"), "tp"),
        P("fs", "tp"),
        P("tp"),
        P("fs", "tp"),
        P("tp", "fs"),
    )

    cut = shape["grp"] == 2 and shape["fs"] == 4 and shape["tp"] == 4

    def body(*blocks):
        if not cut:
            return gathered_weights(*blocks)
        return gathered_tokens(shape["fs"], *blocks)

    return jax.shard_map(
        body, mesh=mesh, in_specs=placed, out_specs=P(("grp", "fs"), "tp"), check_vma=False
    )
```

```python
import functools

import jax
import jax.numpy as jnp
from jax import lax
from jax.experimental import pallas as pl
from jax.experimental.pallas import tpu as pltpu
from jax.sharding import PartitionSpec as P

epsilon = 1e-06


def fold_product(left, portion):
    return jnp.dot(left, portion, preferred_element_type=jnp.float32)


def gathered_weights(stream, mixed, out_weight, norm_gain, up_weight, down_weight):
    mixed_whole = lax.all_gather(mixed, "tp", axis=1, tiled=True)
    projected = fold_product(mixed_whole, lax.all_gather(out_weight, "fs", axis=0, tiled=True))
    resid = (stream.astype(jnp.float32) + projected).astype(jnp.bfloat16)
    widened = resid.astype(jnp.float32)
    resid_whole, gain_whole = (
        lax.all_gather(resid, "tp", axis=1, tiled=True),
        lax.all_gather(norm_gain, "tp", axis=0, tiled=True),
    )
    stream_wide = resid_whole.astype(jnp.float32)
    energy = jnp.mean(stream_wide * stream_wide, axis=1, keepdims=True)
    normed_whole = (
        stream_wide * lax.rsqrt(energy + epsilon) * gain_whole.astype(jnp.float32)
    ).astype(jnp.bfloat16)
    up_full = lax.all_gather(up_weight, "fs", axis=0, tiled=True)
    up_values = fold_product(normed_whole, up_full)
    activated = jnp.square(jax.nn.relu(up_values)).astype(jnp.bfloat16)
    partials = fold_product(activated, lax.all_gather(down_weight, "fs", axis=1, tiled=True))
    branch = lax.psum_scatter(partials, "tp", scatter_dimension=1, tiled=True)
    return (widened + branch).astype(jnp.bfloat16)


def dot_of(left, right):
    return jnp.dot(left, right, preferred_element_type=jnp.float32)


def most_projection_kernel(at, stacked, weight, near1, near2, near3, far1, far2, stream, near, far):
    half = near1.shape[1]
    mine = pl.ds(pl.multiple_of(at[4] * half, half), half)
    other = pl.ds(pl.multiple_of((1 - at[4]) * half, half), half)
    total = dot_of(stacked[at[0]], weight[:, mine])
    for flip, piece in ((1, near1), (2, near2), (3, near3)):
        total += dot_of(stacked[at[flip]], piece[...])
    near[...] = stream[:, mine].astype(jnp.float32) + total
    total = dot_of(stacked[at[0]], weight[:, other])
    for flip, piece in ((1, far1), (2, far2)):
        total += dot_of(stacked[at[flip]], piece[...])
    far[...] = stream[:, other].astype(jnp.float32) + total


def last_projection_kernel(at, stacked, far3, near, far, gain, resid, scaled):
    half = far3.shape[1]
    last = far[...] + dot_of(stacked[at[3]], far3[...])
    for side, value in ((at[4], near[...]), (1 - at[4], last)):
        columns = pl.ds(pl.multiple_of(side * half, half), half)
        kept = value.astype(jnp.bfloat16)
        resid[:, columns] = kept
        scaled[:, columns] = (kept.astype(jnp.float32) * gain[:, columns].astype(jnp.float32)).astype(jnp.bfloat16)


def stack_kernel(own_first, own_second, pair_first, pair_second, out):
    tokens = own_first.shape[0]
    for side, blocks in enumerate(((own_first, own_second), (pair_first, pair_second))):
        for number, block in enumerate(blocks):
            out[side, number * tokens : (number + 1) * tokens, :] = block[...]


def mean_kernel(features, one, two, out):
    out[...] = (one[...] + two[...]) / features


def inverse_kernel(energy, out):
    out[...] = 1.0 / (energy[...] + epsilon)


def hidden_products(mine, others, weights, out):
    depth = mine.shape[2]
    total = None
    for flip in range(4):
        left = (others if flip % 2 else mine)[flip // 2]
        term = dot_of(left, weights[flip * depth : (flip + 1) * depth, :])
        total = term if total is None else total + term
    out[...] = jnp.square(jnp.maximum(total, 0.0)).astype(jnp.bfloat16)


def first_hidden_kernel(place, mine, others, *rest):
    near, far, out, weights = rest[:4], rest[4:6], rest[6], rest[7]
    depth, half = near[0].shape
    for slot, piece in enumerate(near):
        rows = pl.ds(pl.multiple_of(place[slot] * depth, depth), depth)
        weights[rows, :half] = piece[...]
        weights[rows, half:] = far[0][...] if slot == 0 else far[1][slot - 1]
    hidden_products(mine, others, weights, out)


def second_hidden_kernel(mine, others, weights, out):
    hidden_products(mine, others, weights, out)


def branch_products(place, own, other, last, weights, keep, give):
    depth = own.shape[1]
    half = last.shape[0]
    extra = dot_of(jnp.where(place[7] == 0, own[:, half:], other[:, half:]), last[...])
    for side, target in ((1, give), (0, keep)):
        value = dot_of(own, weights[side, :depth, :]) + dot_of(other, weights[side, depth:, :])
        value += jnp.where(place[3] == side, extra, 0.0)
        target[...] = value.astype(target.dtype)


def place_piece(place, weights, slot, far, piece):
    half = piece.shape[0]
    begin = pl.multiple_of(place[4 + slot] * (2 * half) + far * half, half)
    weights[place[slot], pl.ds(begin, half), :] = piece


def place_kernel(place, *rest):
    near, far, weights = rest[:4], rest[4:7], rest[7]
    for side, pieces in enumerate((near, far)):
        for slot, piece in enumerate(pieces):
            place_piece(place, weights, slot, side, piece[...])
    place_piece(place, weights, 3, 1, jnp.zeros_like(near[3]))


def later_branch_kernel(place, own, other, last, weights, *outs):
    some = outs[0].shape[0]
    begin = own.shape[0] // 2
    for number in range(2):
        rows = slice(begin + number * some, begin + (number + 1) * some)
        branch_products(place, own[rows, :], other[rows, :], last, weights, *outs[2 * number : 2 * number + 2])


def both_branch_kernel(place, own, other, last, weights, keep_one, give_one, keep_three, give_three):
    tokens = keep_one.shape[0]
    branch_products(place, own[:tokens, :], other[:tokens, :], last, weights, keep_one, give_one)
    branch_products(place, own[tokens:, :], other[tokens:, :], last, weights, keep_three, give_three)


def first_branch_kernel(place, own, other, last, weights, keep, give):
    tokens = keep.shape[0]
    branch_products(place, own[:tokens, :], other[:tokens, :], last, weights, keep, give)


def pair_sum_kernel(keep, got, out):
    out[...] = (keep[...] + got[...].astype(jnp.float32)).astype(out.dtype)


def cut_kernel(axis, at, whole, *rest):
    outs, sems = rest[:-1], rest[-1]
    copies = []
    for number, out in enumerate(outs):
        size = out.shape[axis]
        span = pl.ds(pl.multiple_of(at[number] * size, size), size)
        source = whole.at[span, :] if axis == 0 else whole.at[:, span]
        copies.append(pltpu.make_async_copy(source, out, sems.at[number]))
        copies[-1].start()
    for copy in copies:
        copy.wait()


def cut(whole, axis, size, starts):
    shape = tuple(size if i == axis else n for i, n in enumerate(whole.shape))
    out = jax.ShapeDtypeStruct(shape, whole.dtype)
    place = jnp.stack([jnp.asarray(x, jnp.int32) for x in starts])
    return pl.pallas_call(
        functools.partial(cut_kernel, axis),
        out_shape=[out] * len(starts),
        in_specs=[pl.BlockSpec(memory_space=pltpu.SMEM), pl.BlockSpec(memory_space=pltpu.HBM)],
        out_specs=[pl.BlockSpec(memory_space=pltpu.VMEM)] * len(starts),
        scratch_shapes=[pltpu.SemaphoreType.DMA((len(starts),))],
        compiler_params=pltpu.CompilerParams(vmem_limit_bytes=4 << 20),
        cost_estimate=pl.CostEstimate(flops=1024, bytes_accessed=1 << 20, transcendentals=0),
    )(place, whole)


def local_call(kernel, outs, *operands, flops, room=8):
    specs = [
        pl.BlockSpec(memory_space=pltpu.SMEM if x.dtype == jnp.int32 else pltpu.VMEM) for x in operands
    ]
    return pl.pallas_call(
        kernel,
        out_shape=outs,
        in_specs=specs,
        out_specs=jax.tree.map(lambda _: pl.BlockSpec(memory_space=pltpu.VMEM), outs),
        compiler_params=pltpu.CompilerParams(vmem_limit_bytes=room << 20),
        cost_estimate=pl.CostEstimate(flops=flops, bytes_accessed=1 << 20, transcendentals=0),
    )(*operands)


def gathered_tokens(parts, stream, mixed, out_weight, norm_gain, up_weight, down_weight):
    tokens, width = stream.shape
    half = width // 2
    unit = up_weight.shape[1] // parts
    part, row, column = lax.axis_index("grp"), lax.axis_index("fs"), lax.axis_index("tp")
    flips = (1, 2, 3)

    def along_rows(value, flip):
        return lax.ppermute(value, "fs", [(i, i ^ flip) for i in range(parts)])

    def across_parts(value):
        return lax.ppermute(value, "grp", [(0, 1), (1, 0)])

    def across_columns(value, flip):
        return lax.ppermute(value, "tp", [(i, i ^ flip) for i in range(parts)])

    at = jnp.stack([column ^ row ^ s for s in range(parts)] + [part]).astype(jnp.int32)
    (out_mine,) = cut(out_weight, 1, half, [part])
    out_near = {s: along_rows(out_mine, s) for s in (1, 2)}
    out_near[3] = along_rows(out_near[2], 1)
    flipped = [across_columns(mixed, flip) for flip in (1, 2, 3)]
    out_far = {s: across_parts(out_near[s]) for s in flips}
    sums = jax.ShapeDtypeStruct((tokens, half), jnp.float32)
    flops = 2 * tokens * width * half
    stacked = jnp.stack([mixed, *flipped])
    near, far = local_call(
        most_projection_kernel, (sums, sums),
        at, stacked, out_weight, *(out_near[s] for s in flips), out_far[1], out_far[2], stream,
        flops=7 * flops,
    )
    resid, scaled = local_call(
        last_projection_kernel,
        (jax.ShapeDtypeStruct((tokens, width), jnp.bfloat16),) * 2,
        at, stacked, out_far[3], near, far, norm_gain.reshape(1, width),
        flops=flops,
    )
    widened = resid.astype(jnp.float32)
    power = jnp.sum(widened * widened, axis=1).reshape(-1, 128)
    power += across_columns(power, 2)
    small = jax.ShapeDtypeStruct(power.shape, jnp.float32)
    energy = local_call(
        functools.partial(mean_kernel, parts * width), small, power, across_columns(power, 1), flops=1024
    )
    inverse = local_call(inverse_kernel, small, energy, flops=1024)

    wanted = [2 * (row ^ s) + part for s in (0, *flips)] + [2 * row + 1 - part]
    up_mine, *up_sent, up_other = cut(up_weight, 1, unit // 2, wanted)
    up_near = {s: along_rows(piece, s) for s, piece in zip(flips, up_sent)}
    up_far = across_parts(jnp.stack([up_near[s] for s in (1, 2, 3)]))
    core = column % 2
    odd_one = (row ^ core) % 2
    down_near, down_far, sides, sources = [], [], [], []
    turns = ((0, 0), (0, 1), (2, 0), (2, 1))
    wanted = [2 * (row ^ (pair + (core ^ turn))) + part for pair, turn in turns]
    down_sent = cut(down_weight, 0, unit // 2, wanted)
    for number, (pair, turn) in enumerate(turns):
        moves = []
        for i in range(parts):
            for j in range(parts):
                moves.append((i * parts + j, (i ^ (pair + (j % 2 ^ turn))) * parts + j // 2 * 2 + i % 2))
        down_near.append(lax.ppermute(down_sent[number], ("fs", "tp"), moves))
        down_far.append(across_parts(down_near[-1]))
        sides.append(((row ^ (pair + odd_one)) != column).astype(jnp.int32))
        sources.append((odd_one ^ turn ^ core).astype(jnp.int32))
    down_place = jnp.stack(sides + sources)
    place = at[:parts]

    pairs = {0: across_columns(scaled, 2)}
    rows = {s: along_rows(scaled, s) for s in (1, 2)}
    rows[3] = along_rows(rows[2], 1)
    pairs |= {s: across_columns(rows[s], 2) for s in flips}
    both = jax.ShapeDtypeStruct((2, 2 * tokens, width), jnp.bfloat16)
    even = local_call(stack_kernel, both, scaled, rows[2], pairs[0], pairs[2], flops=1024)
    odd = local_call(stack_kernel, both, rows[1], rows[3], pairs[1], pairs[3], flops=1024)
    even_others = across_columns(even, 1)
    odd_others = across_columns(odd, 1)
    flops = 4 * tokens * parts * width * unit
    some = jax.ShapeDtypeStruct((2 * tokens, unit), jnp.bfloat16)
    hidden_even, up_whole = local_call(
        first_hidden_kernel,
        (some, jax.ShapeDtypeStruct((parts * width, unit), jnp.bfloat16)),
        place, even, even_others,
        up_mine, up_near[1], up_near[2], up_near[3], up_other, up_far,
        flops=flops,
        room=14,
    )
    hidden_odd = local_call(second_hidden_kernel, some, odd, odd_others, up_whole, flops=flops, room=14)

    block = (tokens, width)
    pair_of = (jax.ShapeDtypeStruct(block, jnp.float32), jax.ShapeDtypeStruct(block, jnp.bfloat16))
    other_even = across_columns(hidden_even, 1)
    other_odd = across_columns(hidden_odd, 1)
    whole = jax.ShapeDtypeStruct((2, 2 * unit, width), jnp.bfloat16)
    down_most = local_call(place_kernel, whole, down_place, *down_near, *down_far[:3], flops=1024, room=14)
    half_of = tuple(jax.ShapeDtypeStruct((tokens // 2, width), x.dtype) for x in pair_of)
    keep_two, give_two, keep_four, give_four = local_call(
        later_branch_kernel, half_of * 2,
        down_place, hidden_even, other_even, down_far[3], down_most,
        flops=flops // 2, room=14,
    )
    keep_one, give_one, keep_three, give_three = local_call(
        both_branch_kernel, pair_of * 2,
        down_place, hidden_odd, other_odd, down_far[3], down_most,
        flops=flops, room=14,
    )
    keep_own, give_own = local_call(
        first_branch_kernel, pair_of,
        down_place, hidden_even, other_even, down_far[3], down_most,
        flops=flops // 2, room=14,
    )

    def summed(keep, give):
        out = jax.ShapeDtypeStruct(keep.shape, jnp.bfloat16)
        return local_call(pair_sum_kernel, out, keep, across_columns(give, 2), flops=1024)

    two = summed(keep_two, give_two)
    four = summed(keep_four, give_four)
    one = summed(keep_one, give_one)
    three = summed(keep_three, give_three)
    branch = keep_own + across_columns(give_own, 2)
    branch += jnp.concatenate([along_rows(two, 2), along_rows(four, 2)])
    branch += along_rows(one, 1)
    branch += along_rows(three, 3)
    return (widened + branch * inverse.reshape(tokens, 1)).astype(jnp.bfloat16)


def solution(mesh):
    shape = mesh.shape
    placed = (
        P(("grp", "fs"), "tp"),
        P(("grp", "fs"), "tp"),
        P("fs", "tp"),
        P("tp"),
        P("fs", "tp"),
        P("tp", "fs"),
    )

    cut = shape["grp"] == 2 and shape["fs"] == 4 and shape["tp"] == 4

    def body(*blocks):
        if not cut:
            return gathered_weights(*blocks)
        return gathered_tokens(shape["fs"], *blocks)

    return jax.shard_map(
        body, mesh=mesh, in_specs=placed, out_specs=P(("grp", "fs"), "tp"), check_vma=False
    )
```
